32 devices in a mesh: sp: 8 (over z, y), tp: 4 (over x, core).
Axes of the slice: x: 2, y: 2, z: 4, core: 2. Of those that a mesh axis runs over, the one named last changes fastest.
Arguments:
- tokens: bfloat16 [3072, 2048], P('sp', 'tp'), may hold values from -6 to 6
- norm_gain: float32 [3, 2048], replicated, may hold values from 0.1 to 1.9
- w_value: bfloat16 [3, 2048, 1024], P(None, 'sp', 'tp'), may hold values from -0.125 to 0.125
- w_gate: bfloat16 [3, 2048, 1024], P(None, 'sp', 'tp'), may hold values from -0.125 to 0.125
- conv_taps: float32 [3, 31, 1024], P(None, None, 'tp'), may hold values from -2.4 to 2.4
- conv_bias: float32 [3, 1024], P(None, 'tp'), may hold values from -3 to 3
- ln_gain: float32 [3, 1024], P(None, 'tp'), may hold values from 0.1 to 1.9
- ln_shift: float32 [3, 1024], P(None, 'tp'), may hold values from -3 to 3
- w_out: bfloat16 [3, 1024, 2048], P(None, 'tp', 'sp'), may hold values from -0.1875 to 0.1875
Outputs:
- stream: bfloat16 [3072, 2048], P('sp', 'tp')
The draws below stay inside these ranges and needn't reach their ends.
All inputs are finite; a program needn't handle non-finite values.
Results may differ from the reference program's by a relative error of at most 0.015.
Values may be sent and summed in bfloat16 or wider, within the bound.
A program may use at most 64 MiB of HBM per device.

```python
import jax
import jax.numpy as jnp
from jax import lax

D = 2048
CONV_CH = 1024
KERNEL = 31
LAYERS = 3
TOKENS = 3072
N_TP = 4


def draw_conv_taps(key, part):
    first_key, second_key, third_key = jax.random.split(key, 3)
    groups = (CONV_CH + 127) // 128
    group_scale = jnp.exp(jax.random.uniform(second_key, (LAYERS, 1, groups), jnp.float32, -1.0, 1.0))
    group_scale = jnp.repeat(group_scale, 128, axis=2)[:, :, :CONV_CH]
    channel_scale = jnp.exp(jax.random.uniform(third_key, (LAYERS, 1, CONV_CH), jnp.float32, -0.2, 0.2))
    raw_taps = jnp.clip(jax.random.normal(first_key, (LAYERS, KERNEL, CONV_CH), jnp.float32), -4.0, 4.0)
    return (raw_taps * group_scale * channel_scale / jnp.sqrt(float(KERNEL))).astype(jnp.float32)


def steps_of(rng, extent, cuts, smallest, top_value):
    gain = 1.0
    for position, parts in cuts:
        heights = jax.random.uniform(jax.random.fold_in(jax.random.fold_in(rng, 6), position), (parts,), jnp.float32, smallest / len(cuts), top_value / len(cuts))
        gain = gain * jnp.repeat(jnp.exp(heights), extent[position] // parts).reshape((-1,) + (1,) * (len(extent) - 1 - position))
    return gain


def scatter_about(rng, shape, scale, most, shards=(), dtype=jnp.bfloat16):
    level = steps_of(rng, shape, shards, -0.22, 0.18) if shards else 1.0
    result = jax.random.normal(rng, shape, jnp.float32) * scale * level
    return jnp.minimum(jnp.maximum(result, -most), most).astype(dtype)


def setup_inputs(seed: int = 0) -> dict:
    key_list = jax.random.split(jax.random.key(seed), 10)
    return {
        "tokens": scatter_about(key_list[0], (TOKENS, D), 1.0, 6.0, ((0, 8), (1, 4))),
        "norm_gain": jnp.clip(1.0 + 0.18 * jax.random.normal(key_list[1], (LAYERS, D), jnp.float32), 0.1, 1.9),
        "w_value": scatter_about(key_list[2], (LAYERS, D, CONV_CH), D ** -0.5, 0.125, ((1, 8), (2, 4))),
        "w_gate": scatter_about(key_list[3], (LAYERS, D, CONV_CH), D ** -0.5, 0.125, ((1, 8), (2, 4))),
        "conv_taps": draw_conv_taps(jax.random.fold_in(key_list[9], 71), 0),
        "conv_bias": scatter_about(key_list[5], (LAYERS, CONV_CH), 0.5, 3.0, ((1, 4),), jnp.float32),
        "ln_gain": jnp.clip(1.0 + 0.18 * jax.random.normal(key_list[6], (LAYERS, CONV_CH), jnp.float32), 0.1, 1.9),
        "ln_shift": scatter_about(key_list[7], (LAYERS, CONV_CH), 0.5, 3.0, ((1, 4),), jnp.float32),
        "w_out": scatter_about(key_list[8], (LAYERS, CONV_CH, D), CONV_CH ** -0.5, 0.1875, ((1, 4), (2, 8))),
    }


norm_floor = 0.01

def reference(tokens, norm_gain, w_value, w_gate, conv_taps, conv_bias, ln_gain, ln_shift, w_out):
    stream = tokens
    reach = KERNEL // 2
    block_width = CONV_CH // N_TP
    for layer_index in range(LAYERS):
        stream_f32 = stream.astype(jnp.float32)
        scale_rows = lax.rsqrt(lax.optimization_barrier(jnp.mean(stream_f32 * stream_f32, axis=-1, keepdims=True)) + norm_floor)
        normed = (stream_f32 * scale_rows * norm_gain[layer_index]).astype(jnp.bfloat16)
        value_rows = jnp.dot(normed, w_value[layer_index], preferred_element_type=jnp.float32)
        gate_rows = jnp.dot(normed, w_gate[layer_index], preferred_element_type=jnp.float32)
        gated_input = (value_rows * jax.nn.sigmoid(gate_rows)).astype(jnp.bfloat16)
        padded = jnp.pad(gated_input, ((reach, reach), (0, 0))).astype(jnp.float32)
        convolved = jnp.zeros((TOKENS, CONV_CH), jnp.float32) + conv_bias[layer_index]
        for offset in range(KERNEL):
            convolved = convolved + conv_taps[layer_index, offset] * padded[offset:offset + TOKENS]
        average = lax.optimization_barrier(jnp.mean(convolved, axis=-1, keepdims=True))
        spread = lax.optimization_barrier(jnp.mean(convolved * convolved, axis=-1, keepdims=True)) - average * average
        activated = jax.nn.silu((convolved - average) * lax.rsqrt(spread + norm_floor) * ln_gain[layer_index] + ln_shift[layer_index]).astype(jnp.bfloat16)
        summed = jnp.zeros((TOKENS, D), jnp.float32)
        for block_index in range(N_TP):
            first = block_index * block_width
            partial_block = jnp.dot(activated[:, first:first + block_width], w_out[layer_index, first:first + block_width], preferred_element_type=jnp.float32).astype(jnp.bfloat16)
            partial_block = lax.optimization_barrier(partial_block)
            summed = summed + partial_block.astype(jnp.float32)
        stream = (stream_f32 + summed).astype(jnp.bfloat16)
    return stream
```

```python
import functools

import jax
import jax.numpy as jnp
from jax import lax
from jax.experimental import pallas as pl
from jax.experimental.pallas import tpu as pltpu
from jax.sharding import PartitionSpec as P

MESH = pl.DeviceIdType.MESH

norm_floor = 0.01


def with_halo(array, sides, width):
    for axis, dim in sides:
        size, length = (lax.axis_size(axis), array.shape[dim])
        up = [(i, (i + 1) % size) for i in range(size - 1)]
        down = [(j, i) for i, j in up]
        last = lax.slice_in_dim(array, length - width, length, axis=dim)
        first = lax.slice_in_dim(array, 0, width, axis=dim)
        before = lax.ppermute(last, axis, up)
        after = lax.ppermute(first, axis, down)
        array = jnp.concatenate([before, array, after], axis=dim)
    return array


def body(tokens, norm_gain, w_value, w_gate, conv_taps, conv_bias, ln_gain, ln_shift, w_out):
    stream = tokens
    layer_count = w_value.shape[0]
    reach = conv_taps.shape[1] // 2
    local_channels = w_value.shape[2]
    channels = local_channels * lax.axis_size("tp")
    tok_rows = tokens.shape[0]
    whole_value, whole_gate = (
        lax.all_gather(w_value, "sp", axis=1, tiled=True),
        lax.all_gather(w_gate, "sp", axis=1, tiled=True),
    )
    whole_out = lax.all_gather(w_out, "sp", axis=2, tiled=True)
    for layer_index in range(layer_count):
        whole_rows = lax.all_gather(stream, "tp", axis=1, tiled=True)
        rows_f32 = whole_rows.astype(jnp.float32)
        scale_rows = lax.rsqrt(jnp.mean(rows_f32 * rows_f32, axis=-1, keepdims=True) + norm_floor)
        normed = (rows_f32 * scale_rows * norm_gain[layer_index]).astype(jnp.bfloat16)
        value_rows = jnp.dot(normed, whole_value[layer_index], preferred_element_type=jnp.float32)
        gate_rows = jnp.dot(normed, whole_gate[layer_index], preferred_element_type=jnp.float32)
        gated_input = (value_rows * jax.nn.sigmoid(gate_rows)).astype(jnp.bfloat16)
        padded = with_halo(gated_input, (("sp", 0),), reach)
        padded = padded.astype(jnp.float32)
        convolved = jnp.zeros((tok_rows, local_channels), jnp.float32) + conv_bias[layer_index]
        for offset in range(2 * reach + 1):
            convolved = (
                convolved + conv_taps[layer_index, offset] * padded[offset : offset + tok_rows]
            )
        moments = lax.psum(
            (
                jnp.sum(convolved, axis=-1, keepdims=True),
                jnp.sum(convolved * convolved, axis=-1, keepdims=True),
            ),
            "tp",
        )
        average = moments[0] / channels
        spread = moments[1] / channels - average * average
        activated = jax.nn.silu(
            (convolved - average) * lax.rsqrt(spread + norm_floor) * ln_gain[layer_index]
            + ln_shift[layer_index]
        ).astype(jnp.bfloat16)
        partial_rows = jnp.dot(
            activated, whole_out[layer_index], preferred_element_type=jnp.float32
        )
        summed = lax.psum_scatter(
            partial_rows.astype(jnp.bfloat16), "tp", scatter_dimension=1, tiled=True
        ).astype(jnp.float32)
        stream = (stream.astype(jnp.float32) + summed).astype(jnp.bfloat16)
    return stream


def fused(
    dims,
    tok, gain_in, wv_in, wg_in, wo_in, taps_in, bias_in, lng_in, lns_in,
    out,
    wvg, wo, taps, bias, lng, lns, stream, gated, conv, acc1, acc2, act,
    part_out, part_in, stat_out, stat_in, stat_m, final_out, final_in,
    loc_sem, ring_send, ring_recv, pair_send, pair_recv,
    tok_send, tok_recv, halo_send, halo_recv, par_send, par_recv,
    px_send, px_recv, st_send, st_recv, fin_send, fin_recv,
):
    n, tp, layers, ntaps, rows, width, chans, pieces = dims
    feats = width // tp
    drows = width // n
    ocols = width // n
    lch = chans // tp
    pch = 2 * lch
    half_rows = rows // 2
    reach = ntaps // 2
    grain = 16
    halo = grain * layers
    window = half_rows + 2 * halo
    main = half_rows + halo
    m = n // 2
    half_feats = width // 2

    sp = lax.axis_index("sp")
    t = lax.axis_index("tp")
    h = lax.rem(t, 2)
    xg = t // 2
    pair = t + 1 - 2 * h
    across = lax.rem(t + 2, tp)
    odd = lax.rem(sp, 2)
    pos = (1 - odd) * (sp // 2) + odd * (n - (sp + 1) // 2)

    def ring_sp(p):
        p = lax.rem(p + 2 * n, n)
        q = p // m
        return (1 - q) * (2 * p) + q * (2 * (n - p) - 1)

    right, left = ring_sp(pos + 1), ring_sp(pos - 1)
    up, down = lax.rem(sp + 1, n), lax.rem(sp + n - 1, n)

    barrier = pltpu.get_barrier_semaphore()
    greet = [(sp, lax.rem(t + j, tp)) for j in range(1, tp)]
    greet += [(up, j) for j in range(tp)] + [(down, j) for j in range(tp)]
    greet += [(right, t), (left, t)]

    def block(layer, kind, origin, side, half=None):
        if kind == 0:
            r = pl.ds(pl.multiple_of(origin * drows, drows), drows)
            if half is None:
                return wvg.at[layer, side, :, r, :]
            return wvg.at[layer, side, half, r, :]
        c = pl.ds(pl.multiple_of(origin * ocols, ocols), ocols)
        if half is None:
            return wo.at[layer, pl.ds(pl.multiple_of(side * lch, lch), lch), c]
        hl = lch // 2
        return wo.at[layer, pl.ds(pl.multiple_of(side * lch + half * hl, hl), hl), c]

    def local_copies(layer, kind):
        if kind == 0:
            r = pl.ds(pl.multiple_of(sp * drows, drows), drows)
            return [
                pltpu.make_async_copy(wv_in.at[layer], wvg.at[layer, h, 0, r, :], loc_sem.at[3 * layer]),
                pltpu.make_async_copy(wg_in.at[layer], wvg.at[layer, h, 1, r, :], loc_sem.at[3 * layer + 1]),
            ]
        return [pltpu.make_async_copy(wo_in.at[layer], block(layer, 1, sp, h), loc_sem.at[3 * layer + 2])]

    def ring_copy(layer, kind, direction, step):
        shift = -(step - 1) if direction == 0 else step - 1
        half = direction if step == m else None
        ref = block(layer, kind, ring_sp(pos + shift), h, half)
        i = ((layer * 2 + kind) * 2 + direction) * m + step - 1
        return pltpu.make_async_remote_copy(
            src_ref=ref, dst_ref=ref, send_sem=ring_send.at[i], recv_sem=ring_recv.at[i],
            device_id=(right if direction == 0 else left, t), device_id_type=MESH)

    def ring_arrival(layer, kind, direction, step, side):
        shift = -step if direction == 0 else step
        half = direction if step == m else None
        return block(layer, kind, ring_sp(pos + shift), side, half)

    def pair_copy(layer, kind, direction, step, side):
        if step == 0:
            ref, j = block(layer, kind, sp, side), 0
        else:
            ref, j = ring_arrival(layer, kind, direction, step, side), direction * m + step
        i = (layer * 2 + kind) * (2 * m + 1) + j
        return pltpu.make_async_remote_copy(
            src_ref=ref, dst_ref=ref, send_sem=pair_send.at[i], recv_sem=pair_recv.at[i],
            device_id=(sp, pair), device_id_type=MESH)

    def send_own(layer, kind):
        for c in local_copies(layer, kind):
            c.wait()
        for d in range(2):
            ring_copy(layer, kind, d, 1).start()
        pair_copy(layer, kind, 0, 0, h).start()

    def relay(layer, kind, step):
        for d in range(2):
            ref = ring_arrival(layer, kind, d, step, h)
            i = ((layer * 2 + kind) * 2 + d) * m + step - 1
            pltpu.make_async_remote_copy(
                src_ref=ref, dst_ref=ref, send_sem=ring_send.at[i], recv_sem=ring_recv.at[i],
                device_id=(right, t), device_id_type=MESH).wait_recv()
            if step < m:
                ring_copy(layer, kind, d, step + 1).start()
            pair_copy(layer, kind, d, step, h).start()

    def pair_wait(layer, kind):
        pair_copy(layer, kind, 0, 0, 1 - h).wait_recv()
        for step in range(1, m + 1):
            for d in range(2):
                pair_copy(layer, kind, d, step, 1 - h).wait_recv()

    tcols = pl.ds(pl.multiple_of(t * feats, feats), feats)

    def window_cols(owner):
        return pl.ds(pl.multiple_of(owner * feats, feats), feats)

    def tok_copy(j):
        dest = lax.rem(t + j, tp)
        dh = lax.rem(dest, 2)
        return pltpu.make_async_remote_copy(
            src_ref=tok.at[pl.ds(pl.multiple_of(dh * (rows - main), grain), main), :],
            dst_ref=stream.at[pl.ds(pl.multiple_of((1 - dh) * halo, grain), main), tcols],
            send_sem=tok_send.at[j - 1], recv_sem=tok_recv.at[j - 1],
            device_id=(sp, dest), device_id_type=MESH)

    def tok_wait(j):
        owner = lax.rem(t + tp - j, tp)
        ref = stream.at[pl.ds(pl.multiple_of((1 - h) * halo, grain), main), window_cols(owner)]
        return pltpu.make_async_remote_copy(
            src_ref=ref, dst_ref=ref, send_sem=tok_send.at[j - 1], recv_sem=tok_recv.at[j - 1],
            device_id=(sp, pair), device_id_type=MESH)

    def halo_copies():
        for g in range(tp // 2):
            yield pltpu.make_async_remote_copy(
                src_ref=tok.at[pl.ds(rows - halo, halo), :], dst_ref=stream.at[pl.ds(0, halo), tcols],
                send_sem=halo_send.at[2 * g], recv_sem=halo_recv.at[t],
                device_id=(up, 2 * g), device_id_type=MESH)
            yield pltpu.make_async_remote_copy(
                src_ref=tok.at[pl.ds(0, halo), :], dst_ref=stream.at[pl.ds(main, halo), tcols],
                send_sem=halo_send.at[2 * g + 1], recv_sem=halo_recv.at[t],
                device_id=(down, 2 * g + 1), device_id_type=MESH)

    def halo_wait(owner):
        ref = stream.at[pl.ds(pl.multiple_of(h * main, grain), halo), owner * feats:(owner + 1) * feats]
        return pltpu.make_async_remote_copy(
            src_ref=ref, dst_ref=ref, send_sem=halo_send.at[0], recv_sem=halo_recv.at[owner],
            device_id=(sp, pair), device_id_type=MESH)

    def param_copies():
        for i, (a, b) in enumerate(((taps_in, taps), (bias_in, bias), (lng_in, lng), (lns_in, lns))):
            yield pltpu.make_async_remote_copy(
                src_ref=a, dst_ref=b.at[h], send_sem=par_send.at[i], recv_sem=par_recv.at[i],
                device_id=(sp, pair), device_id_type=MESH)

    def param_waits():
        for i, (a, b) in enumerate(((taps_in, taps), (bias_in, bias), (lng_in, lng), (lns_in, lns))):
            yield pltpu.make_async_remote_copy(
                src_ref=a, dst_ref=b.at[1 - h], send_sem=par_send.at[i], recv_sem=par_recv.at[i],
                device_id=(sp, pair), device_id_type=MESH)

    for layer in range(layers):
        for kind in range(2):
            for c in local_copies(layer, kind):
                c.start()
    for dev in greet:
        pl.semaphore_signal(barrier, inc=1, device_id=dev, device_id_type=MESH)
    pl.semaphore_wait(barrier, len(greet))

    for c in halo_copies():
        c.start()
    for j in range(1, tp):
        tok_copy(j).start()
    send_own(0, 0)
    for c in param_copies():
        c.start()
    send_own(0, 1)

    stream[pl.ds(pl.multiple_of((1 - h) * halo, grain), main), tcols] = tok[
        pl.ds(pl.multiple_of(h * (rows - main), grain), main), :]
    taps[h] = taps_in[...]
    bias[h] = bias_in[...]
    lng[h] = lng_in[...]
    lns[h] = lns_in[...]
    stat_m[...] = jnp.zeros_like(stat_m)

    first_row = sp * rows + h * half_rows - halo
    total_rows = n * rows

    def project(layer, start, size):
        x = stream[pl.ds(start, size), :].astype(jnp.float32)
        scale = lax.rsqrt(jnp.mean(x * x, axis=-1, keepdims=True) + norm_floor)
        normed = (x * scale * gain_in[layer:layer + 1, :]).astype(jnp.bfloat16)
        row = lax.broadcasted_iota(jnp.int32, (size, lch), 0) + (first_row + start)
        inside = jnp.logical_and(row >= 0, row < total_rows)
        for c in range(2):
            value = jnp.dot(normed, wvg[layer, c, 0], preferred_element_type=jnp.float32)
            gate = jnp.dot(normed, wvg[layer, c, 1], preferred_element_type=jnp.float32)
            g = (value * jax.nn.sigmoid(gate)).astype(jnp.bfloat16).astype(jnp.float32)
            gated[pl.ds(start, size), c * lch:(c + 1) * lch] = jnp.where(inside, g, 0.0)

    def convolve(layer, start, size):
        lanes_per = 128
        per_side = lch // lanes_per
        acc1[...] = jnp.zeros_like(acc1)
        acc2[...] = jnp.zeros_like(acc2)

        def lane_block(b, carry):
            c = b // per_side
            lane = pl.ds(pl.multiple_of(lax.rem(b, per_side) * lanes_per, lanes_per), lanes_per)
            wide = pl.ds(pl.multiple_of(b * lanes_per, lanes_per), lanes_per)
            for r0 in range(0, size, 112 if size % 112 == 0 else (96 if size % 96 == 0 else 128)):
                rs = 112 if size % 112 == 0 else (96 if size % 96 == 0 else 128)
                total = jnp.zeros((rs, lanes_per), jnp.float32) + bias[c, layer:layer + 1, lane]
                for k in range(ntaps):
                    total = total + taps[c, layer, k:k + 1, lane] * gated[
                        start + r0 + k - reach:start + r0 + k - reach + rs, wide]
                conv[r0:r0 + rs, wide] = total
                acc1[r0:r0 + rs, :] += total
                acc2[r0:r0 + rs, :] += total * total
            return carry

        lax.fori_loop(0, 2 * per_side, lane_block, 0)

    def stat_copy(layer):
        return pltpu.make_async_remote_copy(
            src_ref=stat_out.at[layer], dst_ref=stat_in.at[layer], send_sem=st_send.at[layer],
            recv_sem=st_recv.at[layer], device_id=(sp, across), device_id_type=MESH)

    def part_copy(layer, i, r0, size, last):
        r = pl.ds(r0, size)
        if last:
            src = part_out.at[layer, r, pl.ds(pl.multiple_of((1 - xg) * half_feats, half_feats), half_feats)]
            dst = part_in.at[layer, r, pl.ds(pl.multiple_of((1 - xg) * half_feats, half_feats), half_feats)]
        else:
            src, dst = part_out.at[layer, r, :], part_in.at[layer, r, :]
        return pltpu.make_async_remote_copy(
            src_ref=src, dst_ref=dst, send_sem=px_send.at[layer * pieces + i],
            recv_sem=px_recv.at[layer * pieces + i], device_id=(sp, across), device_id_type=MESH)

    for step in range(1, m + 1):
        relay(0, 0, step)
    for j in range(1, tp):
        tok_wait(j).wait_recv()
    for owner in range(tp):
        halo_wait(owner).wait_recv()
    pair_wait(0, 0)
    if layers > 1:
        send_own(1, 0)
    for i in range(2):
        project(0, i * (window // 2), window // 2)
    for c in param_waits():
        c.wait_recv()

    for layer in range(layers):
        last = layer == layers - 1
        start = grain * (layer + 1)
        size = window - 2 * start
        convolve(layer, start, size)
        lane_id = lax.broadcasted_iota(jnp.int32, (size, 128), 1)
        s1 = jnp.sum(acc1[0:size, :], axis=-1, keepdims=True)
        s2 = jnp.sum(acc2[0:size, :], axis=-1, keepdims=True)
        stat_m[0:size, :] = jnp.where(lane_id == 0, s1, jnp.where(lane_id == 1, s2, 0.0))
        mine = jnp.transpose(stat_m[...])
        stat_out[layer] = mine[0:8, :]
        stat_copy(layer).start()
        for step in range(1, m + 1):
            relay(layer, 1, step)
        if layer + 1 < layers:
            send_own(layer + 1, 1)
        stat_copy(layer).wait_recv()
        both = stat_out[layer] + stat_in[layer]
        wide = jnp.concatenate([both, jnp.zeros((120, both.shape[1]), jnp.float32)], axis=0)
        stat_m[...] = jnp.transpose(wide)
        pair_wait(layer, 1)
        piece = size // pieces
        for i in range(pieces):
            r0 = i * piece
            average = stat_m[r0:r0 + piece, 0:1] / chans
            spread = stat_m[r0:r0 + piece, 1:2] / chans - average * average
            scale = lax.rsqrt(spread + norm_floor)
            for c in range(2):
                y = (conv[r0:r0 + piece, c * lch:(c + 1) * lch] - average) * scale
                y = y * lng[c, layer:layer + 1, :] + lns[c, layer:layer + 1, :]
                act[r0:r0 + piece, c * lch:(c + 1) * lch] = (y / (1.0 + jnp.exp(-y))).astype(jnp.bfloat16)
            part_out[layer, r0:r0 + piece, :] = jnp.dot(
                act[r0:r0 + piece, :], wo[layer], preferred_element_type=jnp.float32).astype(jnp.bfloat16)
            part_copy(layer, i, r0, piece, last).start()
        if not last:
            for step in range(1, m + 1):
                relay(layer + 1, 0, step)
            pair_wait(layer + 1, 0)
            if layer + 2 < layers:
                send_own(layer + 2, 0)
            for i in range(pieces):
                r0 = i * piece
                part_copy(layer, i, r0, piece, last).wait_recv()
                w0 = start + r0
                stream[w0:w0 + piece, :] = (
                    stream[w0:w0 + piece, :].astype(jnp.float32)
                    + part_out[layer, r0:r0 + piece, :].astype(jnp.float32)
                    + part_in[layer, r0:r0 + piece, :].astype(jnp.float32)).astype(jnp.bfloat16)
                project(layer + 1, w0, piece)
        else:
            mycols = pl.ds(pl.multiple_of(xg * half_feats, half_feats), half_feats)

            def fin_copy(i, r0):
                return pltpu.make_async_remote_copy(
                    src_ref=final_out.at[pl.ds(r0, piece), pl.ds(pl.multiple_of((1 - h) * feats, feats), feats)],
                    dst_ref=final_in.at[pl.ds(r0, piece), :],
                    send_sem=fin_send.at[i], recv_sem=fin_recv.at[i],
                    device_id=(sp, pair), device_id_type=MESH)

            for i in range(pieces):
                r0 = i * piece
                ref = part_in.at[layer, pl.ds(r0, piece), mycols]
                pltpu.make_async_remote_copy(
                    src_ref=ref, dst_ref=ref, send_sem=px_send.at[layer * pieces + i],
                    recv_sem=px_recv.at[layer * pieces + i], device_id=(sp, across),
                    device_id_type=MESH).wait_recv()
                w0 = start + r0
                final_out[r0:r0 + piece, :] = (
                    stream[w0:w0 + piece, mycols].astype(jnp.float32)
                    + part_out[layer, r0:r0 + piece, mycols].astype(jnp.float32)
                    + part_in[layer, r0:r0 + piece, mycols].astype(jnp.float32)).astype(jnp.bfloat16)
                fin_copy(i, r0).start()
            out[pl.ds(pl.multiple_of(h * half_rows, grain), half_rows), :] = final_out[
                :, pl.ds(pl.multiple_of(h * feats, feats), feats)]
            for i in range(pieces):
                fin_copy(i, i * piece).wait_recv()
            out[pl.ds(pl.multiple_of((1 - h) * half_rows, grain), half_rows), :] = final_in[...]
            for i in range(pieces):
                fin_copy(i, i * piece).wait_send()

    for c in halo_copies():
        c.wait_send()
    for j in range(1, tp):
        tok_copy(j).wait_send()
    for c in param_copies():
        c.wait_send()
    for layer in range(layers):
        last = layer == layers - 1
        size = window - 2 * grain * (layer + 1)
        piece = size // pieces
        stat_copy(layer).wait_send()
        for i in range(pieces):
            part_copy(layer, i, i * piece, piece, last).wait_send()
        for kind in range(2):
            pair_copy(layer, kind, 0, 0, h).wait_send()
            for step in range(1, m + 1):
                for d in range(2):
                    ring_copy(layer, kind, d, step).wait_send()
                    pair_copy(layer, kind, d, step, h).wait_send()


def fused_call(mesh, *args):
    tokens, norm_gain, w_value, w_gate, conv_taps, conv_bias, ln_gain, ln_shift, w_out = args
    n, tp = mesh.shape["sp"], mesh.shape["tp"]
    layers, ntaps, lch = conv_taps.shape
    rows, feats = tokens.shape
    width, chans = feats * tp, lch * tp
    pieces = 2
    half_rows = rows // 2
    window = half_rows + 32 * layers
    most = window - 32
    stat_rows = -(-most // 128) * 128
    m = n // 2
    dims = (n, tp, layers, ntaps, rows, width, chans, pieces)
    vmem = pl.BlockSpec(memory_space=pltpu.VMEM)
    anys = pl.BlockSpec(memory_space=pl.ANY)
    bf, f32 = jnp.bfloat16, jnp.float32
    dma = lambda k: pltpu.SemaphoreType.DMA((k,))
    ring_sems = layers * 2 * 2 * m
    pair_sems = layers * 2 * (2 * m + 1)
    return pl.pallas_call(
        functools.partial(fused, dims),
        out_shape=jax.ShapeDtypeStruct((rows, feats), bf),
        in_specs=[vmem, vmem, anys, anys, anys, vmem, vmem, vmem, vmem],
        out_specs=vmem,
        scratch_shapes=[
            pltpu.VMEM((layers, 2, 2, width, lch), bf),
            pltpu.VMEM((layers, 2 * lch, width), bf),
            pltpu.VMEM((2,) + conv_taps.shape, f32),
            pltpu.VMEM((2,) + conv_bias.shape, f32),
            pltpu.VMEM((2,) + ln_gain.shape, f32),
            pltpu.VMEM((2,) + ln_shift.shape, f32),
            pltpu.VMEM((window, width), bf),
            pltpu.VMEM((window, 2 * lch), f32),
            pltpu.VMEM((most, 2 * lch), f32),
            pltpu.VMEM((most, 128), f32),
            pltpu.VMEM((most, 128), f32),
            pltpu.VMEM((most, 2 * lch), bf),
            pltpu.VMEM((layers, most, width), bf),
            pltpu.VMEM((layers, most, width), bf),
            pltpu.VMEM((layers, 8, stat_rows), f32),
            pltpu.VMEM((layers, 8, stat_rows), f32),
            pltpu.VMEM((stat_rows, 128), f32),
            pltpu.VMEM((half_rows, 2 * feats), bf),
            pltpu.VMEM((half_rows, feats), bf),
            dma(3 * layers), dma(ring_sems), dma(ring_sems), dma(pair_sems), dma(pair_sems),
            dma(tp - 1), dma(tp - 1), dma(tp), dma(tp), dma(4), dma(4),
            dma(layers * pieces), dma(layers * pieces), dma(layers), dma(layers),
            dma(pieces), dma(pieces),
        ],
        compiler_params=pltpu.CompilerParams(
            collective_id=0, has_side_effects=True, vmem_limit_bytes=60 * 1024 * 1024),
    )(tokens, norm_gain, w_value, w_gate, w_out, conv_taps, conv_bias, ln_gain, ln_shift)


def fits(mesh, tokens, conv_taps, w_out):
    n, tp = mesh.shape["sp"], mesh.shape["tp"]
    layers, ntaps, lch = conv_taps.shape
    rows, feats = tokens.shape
    sizes = [rows // 2 + 32 * (layers - 1 - i) for i in range(layers)]
    return (tp == 4 and n % 2 == 0 and n >= 4 and ntaps % 2 == 1 and ntaps // 2 < 16
            and w_out.shape[2] % 128 == 0 and lch % 256 == 0 and feats % 128 == 0
            and rows % 32 == 0 and rows // 2 >= 16 * layers
            and all(s % 32 == 0 and (s % 112 == 0 or s % 96 == 0 or s % 128 == 0) for s in sizes)
            and layers * w_out.shape[1] * w_out.shape[2] * n * 12 <= 20 * 1024 * 1024)


def solution(mesh):
    placed = (
        P("sp", "tp"),
        P(),
        P(None, "sp", "tp"),
        P(None, "sp", "tp"),
        P(None, None, "tp"),
        P(None, "tp"),
        P(None, "tp"),
        P(None, "tp"),
        P(None, "tp", "sp"),
    )

    def run(*args):
        if fits(mesh, args[0], args[4], args[8]):
            return fused_call(mesh, *args)
        return body(*args)

    return jax.shard_map(run, mesh=mesh, in_specs=placed, out_specs=P("sp", "tp"), check_vma=False)
```

```python
import functools

import jax
import jax.numpy as jnp
from jax import lax
from jax.experimental import pallas as pl
from jax.experimental.pallas import tpu as pltpu
from jax.sharding import PartitionSpec as P

MESH = pl.DeviceIdType.MESH

norm_floor = 0.01


def with_halo(array, sides, width):
    for axis, dim in sides:
        size, length = (lax.axis_size(axis), array.shape[dim])
        up = [(i, (i + 1) % size) for i in range(size - 1)]
        down = [(j, i) for i, j in up]
        last = lax.slice_in_dim(array, length - width, length, axis=dim)
        first = lax.slice_in_dim(array, 0, width, axis=dim)
        before = lax.ppermute(last, axis, up)
        after = lax.ppermute(first, axis, down)
        array = jnp.concatenate([before, array, after], axis=dim)
    return array


def body(tokens, norm_gain, w_value, w_gate, conv_taps, conv_bias, ln_gain, ln_shift, w_out):
    stream = tokens
    layer_count = w_value.shape[0]
    reach = conv_taps.shape[1] // 2
    local_channels = w_value.shape[2]
    channels = local_channels * lax.axis_size("tp")
    tok_rows = tokens.shape[0]
    whole_value, whole_gate = (
        lax.all_gather(w_value, "sp", axis=1, tiled=True),
        lax.all_gather(w_gate, "sp", axis=1, tiled=True),
    )
    whole_out = lax.all_gather(w_out, "sp", axis=2, tiled=True)
    for layer_index in range(layer_count):
        whole_rows = lax.all_gather(stream, "tp", axis=1, tiled=True)
        rows_f32 = whole_rows.astype(jnp.float32)
        scale_rows = lax.rsqrt(jnp.mean(rows_f32 * rows_f32, axis=-1, keepdims=True) + norm_floor)
        normed = (rows_f32 * scale_rows * norm_gain[layer_index]).astype(jnp.bfloat16)
        value_rows = jnp.dot(normed, whole_value[layer_index], preferred_element_type=jnp.float32)
        gate_rows = jnp.dot(normed, whole_gate[layer_index], preferred_element_type=jnp.float32)
        gated_input = (value_rows * jax.nn.sigmoid(gate_rows)).astype(jnp.bfloat16)
        padded = with_halo(gated_input, (("sp", 0),), reach)
        padded = padded.astype(jnp.float32)
        convolved = jnp.zeros((tok_rows, local_channels), jnp.float32) + conv_bias[layer_index]
        for offset in range(2 * reach + 1):
            convolved = (
                convolved + conv_taps[layer_index, offset] * padded[offset : offset + tok_rows]
            )
        moments = lax.psum(
            (
                jnp.sum(convolved, axis=-1, keepdims=True),
                jnp.sum(convolved * convolved, axis=-1, keepdims=True),
            ),
            "tp",
        )
        average = moments[0] / channels
        spread = moments[1] / channels - average * average
        activated = jax.nn.silu(
            (convolved - average) * lax.rsqrt(spread + norm_floor) * ln_gain[layer_index]
            + ln_shift[layer_index]
        ).astype(jnp.bfloat16)
        partial_rows = jnp.dot(
            activated, whole_out[layer_index], preferred_element_type=jnp.float32
        )
        summed = lax.psum_scatter(
            partial_rows.astype(jnp.bfloat16), "tp", scatter_dimension=1, tiled=True
        ).astype(jnp.float32)
        stream = (stream.astype(jnp.float32) + summed).astype(jnp.bfloat16)
    return stream


def ring_order(layers, m):
    order = [(0, 0, 1), (0, 1, 1)]
    for layer in range(layers):
        order.append((layer, 2, 1))
        for step in range(2, m + 1):
            order += [(layer, 0, step), (layer, 1, step)]
        ahead = [(layer + 1, 0, 1), (layer + 1, 1, 1)] if layer + 1 < layers else []
        for step in range(2, m + 1):
            order.append((layer, 2, step))
            order += ahead[:1]
            ahead = ahead[1:]
        order += ahead
    if m > 2:
        last = layers - 1
        early = [(last, 2, step) for step in range(2, m)]
        order = [e for e in order if e not in early]
        for e in early:
            order.insert(order.index((last, 1, e[2] + 1)), e)
    return order


def fused(
    dims,
    tok, gain_in, wv_in, wg_in, wo_in, taps_in, bias_in, lng_in, lns_in,
    out,
    wvg, wo, taps, bias, lng, lns, stream, gated, conv, acc1, acc2, act,
    part_out, part_in, stat_out, stat_in, stat_m, final_out, final_in,
    loc_sem, ring_send, ring_recv, pair_send, pair_recv,
    tok_send, tok_recv, halo_send, halo_recv, par_send, par_recv,
    px_send, px_recv, st_send, st_recv, fin_send, fin_recv,
):
    n, tp, layers, ntaps, rows, width, chans, pieces = dims
    feats = width // tp
    drows = width // n
    ocols = width // n
    lch = chans // tp
    pch = 2 * lch
    half_rows = rows // 2
    reach = ntaps // 2
    grain = 16
    halo = grain * layers
    window = half_rows + 2 * halo
    main = half_rows + halo
    m = n // 2
    half_feats = width // 2

    sp = lax.axis_index("sp")
    t = lax.axis_index("tp")
    h = lax.rem(t, 2)
    xg = t // 2
    pair = t + 1 - 2 * h
    across = lax.rem(t + 2, tp)
    odd = lax.rem(sp, 2)
    pos = (1 - odd) * (sp // 2) + odd * (n - (sp + 1) // 2)

    def ring_sp(p):
        p = lax.rem(p + 2 * n, n)
        q = p // m
        return (1 - q) * (2 * p) + q * (2 * (n - p) - 1)

    right, left = ring_sp(pos + 1), ring_sp(pos - 1)
    up, down = lax.rem(sp + 1, n), lax.rem(sp + n - 1, n)

    barrier = pltpu.get_barrier_semaphore()
    greet = [(sp, lax.rem(t + j, tp)) for j in range(1, tp)]
    greet += [(up, j) for j in range(tp)] + [(down, j) for j in range(tp)]
    greet += [(right, t), (left, t)]

    def block(layer, kind, origin, side, half=None):
        part, count = (0, 1) if half is None else (half, 2)
        if kind < 2:
            size = drows // count
            r = pl.ds(pl.multiple_of(origin * drows + part * size, size), size)
            return wvg.at[layer, side, kind, r, :]
        size = lch // count
        c = pl.ds(pl.multiple_of(origin * ocols, ocols), ocols)
        return wo.at[layer, pl.ds(pl.multiple_of(side * lch + part * size, size), size), c]

    def local_copy(layer, kind):
        src = (wv_in, wg_in, wo_in)[kind].at[layer]
        return pltpu.make_async_copy(src, block(layer, kind, sp, h), loc_sem.at[3 * layer + kind])

    def ring_copy(layer, kind, direction, step):
        shift = -(step - 1) if direction == 0 else step - 1
        half = direction if step == m else None
        ref = block(layer, kind, ring_sp(pos + shift), h, half)
        i = ((layer * 3 + kind) * 2 + direction) * m + step - 1
        return pltpu.make_async_remote_copy(
            src_ref=ref, dst_ref=ref, send_sem=ring_send.at[i], recv_sem=ring_recv.at[i],
            device_id=(right if direction == 0 else left, t), device_id_type=MESH)

    def ring_arrival(layer, kind, direction, step, side):
        shift = -step if direction == 0 else step
        half = direction if step == m else None
        return block(layer, kind, ring_sp(pos + shift), side, half)

    def pair_copy(layer, kind, direction, step, side):
        if step == 0:
            ref, j = block(layer, kind, sp, side), 0
        else:
            ref, j = ring_arrival(layer, kind, direction, step, side), direction * m + step
        i = (layer * 3 + kind) * (2 * m + 1) + j
        return pltpu.make_async_remote_copy(
            src_ref=ref, dst_ref=ref, send_sem=pair_send.at[i], recv_sem=pair_recv.at[i],
            device_id=(sp, pair), device_id_type=MESH)

    sequence = ring_order(layers, m)
    place = {e: i for i, e in enumerate(sequence)}
    sent, handled = [0], [0]

    def pump():
        while sent[0] < len(sequence):
            layer, kind, step = sequence[sent[0]]
            if step > 1 and place[layer, kind, step - 1] >= handled[0]:
                return
            if step == 1:
                local_copy(layer, kind).wait()
            for d in range(2):
                ring_copy(layer, kind, d, step).start()
            if step == 1:
                pair_copy(layer, kind, 0, 0, h).start()
            sent[0] += 1

    def advance(upto):
        while handled[0] < min(upto, len(sequence)):
            layer, kind, step = sequence[handled[0]]
            for d in range(2):
                ref = ring_arrival(layer, kind, d, step, h)
                i = ((layer * 3 + kind) * 2 + d) * m + step - 1
                pltpu.make_async_remote_copy(
                    src_ref=ref, dst_ref=ref, send_sem=ring_send.at[i], recv_sem=ring_recv.at[i],
                    device_id=(right, t), device_id_type=MESH).wait_recv()
            handled[0] += 1
            pump()
            for d in range(2):
                pair_copy(layer, kind, d, step, h).start()

    def advance_by(count):
        advance(handled[0] + count)

    def need(layer, *kinds):
        advance(max(place[layer, k, m] for k in kinds) + 1)
        for k in kinds:
            pair_copy(layer, k, 0, 0, 1 - h).wait_recv()
            for step in range(1, m + 1):
                for d in range(2):
                    pair_copy(layer, k, d, step, 1 - h).wait_recv()

    tcols = pl.ds(pl.multiple_of(t * feats, feats), feats)

    def window_cols(owner):
        return pl.ds(pl.multiple_of(owner * feats, feats), feats)

    def tok_copy(j):
        dest = lax.rem(t + j, tp)
        dh = lax.rem(dest, 2)
        return pltpu.make_async_remote_copy(
            src_ref=tok.at[pl.ds(pl.multiple_of(dh * (rows - main), grain), main), :],
            dst_ref=stream.at[pl.ds(pl.multiple_of((1 - dh) * halo, grain), main), tcols],
            send_sem=tok_send.at[j - 1], recv_sem=tok_recv.at[j - 1],
            device_id=(sp, dest), device_id_type=MESH)

    def tok_wait(j):
        owner = lax.rem(t + tp - j, tp)
        ref = stream.at[pl.ds(pl.multiple_of((1 - h) * halo, grain), main), window_cols(owner)]
        return pltpu.make_async_remote_copy(
            src_ref=ref, dst_ref=ref, send_sem=tok_send.at[j - 1], recv_sem=tok_recv.at[j - 1],
            device_id=(sp, pair), device_id_type=MESH)

    def halo_copies():
        for g in range(tp // 2):
            yield pltpu.make_async_remote_copy(
                src_ref=tok.at[pl.ds(rows - halo, halo), :], dst_ref=stream.at[pl.ds(0, halo), tcols],
                send_sem=halo_send.at[2 * g], recv_sem=halo_recv.at[t],
                device_id=(up, 2 * g), device_id_type=MESH)
            yield pltpu.make_async_remote_copy(
                src_ref=tok.at[pl.ds(0, halo), :], dst_ref=stream.at[pl.ds(main, halo), tcols],
                send_sem=halo_send.at[2 * g + 1], recv_sem=halo_recv.at[t],
                device_id=(down, 2 * g + 1), device_id_type=MESH)

    def halo_wait(owner):
        ref = stream.at[pl.ds(pl.multiple_of(h * main, grain), halo), owner * feats:(owner + 1) * feats]
        return pltpu.make_async_remote_copy(
            src_ref=ref, dst_ref=ref, send_sem=halo_send.at[0], recv_sem=halo_recv.at[owner],
            device_id=(sp, pair), device_id_type=MESH)

    def param_copies():
        for i, (a, b) in enumerate(((taps_in, taps), (bias_in, bias), (lng_in, lng), (lns_in, lns))):
            yield pltpu.make_async_remote_copy(
                src_ref=a, dst_ref=b.at[h], send_sem=par_send.at[i], recv_sem=par_recv.at[i],
                device_id=(sp, pair), device_id_type=MESH)

    def param_waits():
        for i, (a, b) in enumerate(((taps_in, taps), (bias_in, bias), (lng_in, lng), (lns_in, lns))):
            yield pltpu.make_async_remote_copy(
                src_ref=a, dst_ref=b.at[1 - h], send_sem=par_send.at[i], recv_sem=par_recv.at[i],
                device_id=(sp, pair), device_id_type=MESH)

    for layer in range(layers):
        for kind in range(3):
            local_copy(layer, kind).start()
    for dev in greet:
        pl.semaphore_signal(barrier, inc=1, device_id=dev, device_id_type=MESH)
    pl.semaphore_wait(barrier, len(greet))

    pump()
    for j in range(1, tp):
        tok_copy(j).start()
    for c in halo_copies():
        c.start()
    for c in param_copies():
        c.start()

    stream[pl.ds(pl.multiple_of((1 - h) * halo, grain), main), tcols] = tok[
        pl.ds(pl.multiple_of(h * (rows - main), grain), main), :]
    taps[h] = taps_in[...]
    bias[h] = bias_in[...]
    lng[h] = lng_in[...]
    lns[h] = lns_in[...]
    stat_m[...] = jnp.zeros_like(stat_m)

    first_row = sp * rows + h * half_rows - halo
    total_rows = n * rows

    def project(layer, start, size):
        x = stream[pl.ds(start, size), :].astype(jnp.float32)
        scale = lax.rsqrt(jnp.mean(x * x, axis=-1, keepdims=True) + norm_floor)
        normed = (x * scale * gain_in[layer:layer + 1, :]).astype(jnp.bfloat16)
        row = lax.broadcasted_iota(jnp.int32, (size, lch), 0) + (first_row + start)
        inside = jnp.logical_and(row >= 0, row < total_rows)
        for c in range(2):
            value = jnp.dot(normed, wvg[layer, c, 0], preferred_element_type=jnp.float32)
            gate = jnp.dot(normed, wvg[layer, c, 1], preferred_element_type=jnp.float32)
            g = (value * jax.nn.sigmoid(gate)).astype(jnp.bfloat16).astype(jnp.float32)
            gated[pl.ds(start, size), c * lch:(c + 1) * lch] = jnp.where(inside, g, 0.0)

    def convolve(layer, start, size):
        lanes_per = 128
        per_side = lch // lanes_per
        acc1[...] = jnp.zeros_like(acc1)
        acc2[...] = jnp.zeros_like(acc2)

        def lane_block(b, carry):
            c = b // per_side
            lane = pl.ds(pl.multiple_of(lax.rem(b, per_side) * lanes_per, lanes_per), lanes_per)
            wide = pl.ds(pl.multiple_of(b * lanes_per, lanes_per), lanes_per)
            for r0 in range(0, size, 112 if size % 112 == 0 else (96 if size % 96 == 0 else 128)):
                rs = 112 if size % 112 == 0 else (96 if size % 96 == 0 else 128)
                total = jnp.zeros((rs, lanes_per), jnp.float32) + bias[c, layer:layer + 1, lane]
                for k in range(ntaps):
                    total = total + taps[c, layer, k:k + 1, lane] * gated[
                        start + r0 + k - reach:start + r0 + k - reach + rs, wide]
                conv[r0:r0 + rs, wide] = total
                acc1[r0:r0 + rs, :] += total
                acc2[r0:r0 + rs, :] += total * total
            return carry

        lax.fori_loop(0, 2 * per_side, lane_block, 0)

    def stat_copy(layer):
        return pltpu.make_async_remote_copy(
            src_ref=stat_out.at[layer], dst_ref=stat_in.at[layer], send_sem=st_send.at[layer],
            recv_sem=st_recv.at[layer], device_id=(sp, across), device_id_type=MESH)

    def part_copy(layer, i, r0, size, last):
        r = pl.ds(r0, size)
        if last:
            src = part_out.at[layer, r, pl.ds(pl.multiple_of((1 - xg) * half_feats, half_feats), half_feats)]
            dst = part_in.at[layer, r, pl.ds(pl.multiple_of((1 - xg) * half_feats, half_feats), half_feats)]
        else:
            src, dst = part_out.at[layer, r, :], part_in.at[layer, r, :]
        return pltpu.make_async_remote_copy(
            src_ref=src, dst_ref=dst, send_sem=px_send.at[layer * pieces + i],
            recv_sem=px_recv.at[layer * pieces + i], device_id=(sp, across), device_id_type=MESH)

    advance(max(place[0, 0, m], place[0, 1, m]) + 1)
    for j in range(1, tp):
        tok_wait(j).wait_recv()
    for owner in range(tp):
        halo_wait(owner).wait_recv()
    need(0, 0, 1)
    for i in range(2):
        project(0, i * (window // 2), window // 2)
    advance_by(1)
    for c in param_waits():
        c.wait_recv()

    for layer in range(layers):
        last = layer == layers - 1
        start = grain * (layer + 1)
        size = window - 2 * start
        convolve(layer, start, size)
        advance_by(1)
        lane_id = lax.broadcasted_iota(jnp.int32, (size, 128), 1)
        s1 = jnp.sum(acc1[0:size, :], axis=-1, keepdims=True)
        s2 = jnp.sum(acc2[0:size, :], axis=-1, keepdims=True)
        stat_m[0:size, :] = jnp.where(lane_id == 0, s1, jnp.where(lane_id == 1, s2, 0.0))
        mine = jnp.transpose(stat_m[...])
        stat_out[layer] = mine[0:8, :]
        stat_copy(layer).start()
        advance(place[layer, 2, m] + 1)
        stat_copy(layer).wait_recv()
        both = stat_out[layer] + stat_in[layer]
        wide = jnp.concatenate([both, jnp.zeros((120, both.shape[1]), jnp.float32)], axis=0)
        stat_m[...] = jnp.transpose(wide)
        need(layer, 2)
        piece = size // pieces
        for i in range(pieces):
            r0 = i * piece
            average = stat_m[r0:r0 + piece, 0:1] / chans
            spread = stat_m[r0:r0 + piece, 1:2] / chans - average * average
            scale = lax.rsqrt(spread + norm_floor)
            for c in range(2):
                y = (conv[r0:r0 + piece, c * lch:(c + 1) * lch] - average) * scale
                y = y * lng[c, layer:layer + 1, :] + lns[c, layer:layer + 1, :]
                act[r0:r0 + piece, c * lch:(c + 1) * lch] = (y / (1.0 + jnp.exp(-y))).astype(jnp.bfloat16)
            part_out[layer, r0:r0 + piece, :] = jnp.dot(
                act[r0:r0 + piece, :], wo[layer], preferred_element_type=jnp.float32).astype(jnp.bfloat16)
            part_copy(layer, i, r0, piece, last).start()
        if not last:
            need(layer + 1, 0, 1)
            for i in range(pieces):
                r0 = i * piece
                part_copy(layer, i, r0, piece, last).wait_recv()
                w0 = start + r0
                stream[w0:w0 + piece, :] = (
                    stream[w0:w0 + piece, :].astype(jnp.float32)
                    + part_out[layer, r0:r0 + piece, :].astype(jnp.float32)
                    + part_in[layer, r0:r0 + piece, :].astype(jnp.float32)).astype(jnp.bfloat16)
                project(layer + 1, w0, piece)
                advance_by(1)
        else:
            mycols = pl.ds(pl.multiple_of(xg * half_feats, half_feats), half_feats)

            def fin_copy(i, r0):
                return pltpu.make_async_remote_copy(
                    src_ref=final_out.at[pl.ds(r0, piece), pl.ds(pl.multiple_of((1 - h) * feats, feats), feats)],
                    dst_ref=final_in.at[pl.ds(r0, piece), :],
                    send_sem=fin_send.at[i], recv_sem=fin_recv.at[i],
                    device_id=(sp, pair), device_id_type=MESH)

            for i in range(pieces):
                r0 = i * piece
                ref = part_in.at[layer, pl.ds(r0, piece), mycols]
                pltpu.make_async_remote_copy(
                    src_ref=ref, dst_ref=ref, send_sem=px_send.at[layer * pieces + i],
                    recv_sem=px_recv.at[layer * pieces + i], device_id=(sp, across),
                    device_id_type=MESH).wait_recv()
                w0 = start + r0
                final_out[r0:r0 + piece, :] = (
                    stream[w0:w0 + piece, mycols].astype(jnp.float32)
                    + part_out[layer, r0:r0 + piece, mycols].astype(jnp.float32)
                    + part_in[layer, r0:r0 + piece, mycols].astype(jnp.float32)).astype(jnp.bfloat16)
                fin_copy(i, r0).start()
            out[pl.ds(pl.multiple_of(h * half_rows, grain), half_rows), :] = final_out[
                :, pl.ds(pl.multiple_of(h * feats, feats), feats)]
            for i in range(pieces):
                fin_copy(i, i * piece).wait_recv()
            out[pl.ds(pl.multiple_of((1 - h) * half_rows, grain), half_rows), :] = final_in[...]
            for i in range(pieces):
                fin_copy(i, i * piece).wait_send()

    for c in halo_copies():
        c.wait_send()
    for j in range(1, tp):
        tok_copy(j).wait_send()
    for c in param_copies():
        c.wait_send()
    for layer in range(layers):
        last = layer == layers - 1
        size = window - 2 * grain * (layer + 1)
        piece = size // pieces
        stat_copy(layer).wait_send()
        for i in range(pieces):
            part_copy(layer, i, i * piece, piece, last).wait_send()
        for kind in range(3):
            pair_copy(layer, kind, 0, 0, h).wait_send()
            for step in range(1, m + 1):
                for d in range(2):
                    ring_copy(layer, kind, d, step).wait_send()
                    pair_copy(layer, kind, d, step, h).wait_send()


def fused_call(mesh, *args):
    tokens, norm_gain, w_value, w_gate, conv_taps, conv_bias, ln_gain, ln_shift, w_out = args
    n, tp = mesh.shape["sp"], mesh.shape["tp"]
    layers, ntaps, lch = conv_taps.shape
    rows, feats = tokens.shape
    width, chans = feats * tp, lch * tp
    pieces = 2
    half_rows = rows // 2
    window = half_rows + 32 * layers
    most = window - 32
    stat_rows = -(-most // 128) * 128
    m = n // 2
    dims = (n, tp, layers, ntaps, rows, width, chans, pieces)
    vmem = pl.BlockSpec(memory_space=pltpu.VMEM)
    anys = pl.BlockSpec(memory_space=pl.ANY)
    bf, f32 = jnp.bfloat16, jnp.float32
    dma = lambda k: pltpu.SemaphoreType.DMA((k,))
    ring_sems = layers * 3 * 2 * m
    pair_sems = layers * 3 * (2 * m + 1)
    return pl.pallas_call(
        functools.partial(fused, dims),
        out_shape=jax.ShapeDtypeStruct((rows, feats), bf),
        in_specs=[vmem, vmem, anys, anys, anys, vmem, vmem, vmem, vmem],
        out_specs=vmem,
        scratch_shapes=[
            pltpu.VMEM((layers, 2, 2, width, lch), bf),
            pltpu.VMEM((layers, 2 * lch, width), bf),
            pltpu.VMEM((2,) + conv_taps.shape, f32),
            pltpu.VMEM((2,) + conv_bias.shape, f32),
            pltpu.VMEM((2,) + ln_gain.shape, f32),
            pltpu.VMEM((2,) + ln_shift.shape, f32),
            pltpu.VMEM((window, width), bf),
            pltpu.VMEM((window, 2 * lch), f32),
            pltpu.VMEM((most, 2 * lch), f32),
            pltpu.VMEM((most, 128), f32),
            pltpu.VMEM((most, 128), f32),
            pltpu.VMEM((most, 2 * lch), bf),
            pltpu.VMEM((layers, most, width), bf),
            pltpu.VMEM((layers, most, width), bf),
            pltpu.VMEM((layers, 8, stat_rows), f32),
            pltpu.VMEM((layers, 8, stat_rows), f32),
            pltpu.VMEM((stat_rows, 128), f32),
            pltpu.VMEM((half_rows, 2 * feats), bf),
            pltpu.VMEM((half_rows, feats), bf),
            dma(3 * layers), dma(ring_sems), dma(ring_sems), dma(pair_sems), dma(pair_sems),
            dma(tp - 1), dma(tp - 1), dma(tp), dma(tp), dma(4), dma(4),
            dma(layers * pieces), dma(layers * pieces), dma(layers), dma(layers),
            dma(pieces), dma(pieces),
        ],
        compiler_params=pltpu.CompilerParams(
            collective_id=0, has_side_effects=True, vmem_limit_bytes=60 * 1024 * 1024),
    )(tokens, norm_gain, w_value, w_gate, w_out, conv_taps, conv_bias, ln_gain, ln_shift)


def fits(mesh, tokens, conv_taps, w_out):
    n, tp = mesh.shape["sp"], mesh.shape["tp"]
    layers, ntaps, lch = conv_taps.shape
    rows, feats = tokens.shape
    sizes = [rows // 2 + 32 * (layers - 1 - i) for i in range(layers)]
    return (tp == 4 and n % 2 == 0 and n >= 4 and ntaps % 2 == 1 and ntaps // 2 < 16
            and w_out.shape[2] % 128 == 0 and lch % 256 == 0 and feats % 128 == 0
            and rows % 32 == 0 and rows // 2 >= 16 * layers
            and all(s % 32 == 0 and (s % 112 == 0 or s % 96 == 0 or s % 128 == 0) for s in sizes)
            and layers * w_out.shape[1] * w_out.shape[2] * n * 12 <= 20 * 1024 * 1024)


def solution(mesh):
    placed = (
        P("sp", "tp"),
        P(),
        P(None, "sp", "tp"),
        P(None, "sp", "tp"),
        P(None, None, "tp"),
        P(None, "tp"),
        P(None, "tp"),
        P(None, "tp"),
        P(None, "tp", "sp"),
    )

    def run(*args):
        if fits(mesh, args[0], args[4], args[8]):
            return fused_call(mesh, *args)
        return body(*args)

    return jax.shard_map(run, mesh=mesh, in_specs=placed, out_specs=P("sp", "tp"), check_vma=False)
```

```python
import functools

import jax
import jax.numpy as jnp
from jax import lax
from jax.experimental import pallas as pl
from jax.experimental.pallas import tpu as pltpu
from jax.sharding import PartitionSpec as P

MESH = pl.DeviceIdType.MESH

norm_floor = 0.01


def with_halo(array, sides, width):
    for axis, dim in sides:
        size, length = (lax.axis_size(axis), array.shape[dim])
        up = [(i, (i + 1) % size) for i in range(size - 1)]
        down = [(j, i) for i, j in up]
        last = lax.slice_in_dim(array, length - width, length, axis=dim)
        first = lax.slice_in_dim(array, 0, width, axis=dim)
        before = lax.ppermute(last, axis, up)
        after = lax.ppermute(first, axis, down)
        array = jnp.concatenate([before, array, after], axis=dim)
    return array


def body(tokens, norm_gain, w_value, w_gate, conv_taps, conv_bias, ln_gain, ln_shift, w_out):
    stream = tokens
    layer_count = w_value.shape[0]
    reach = conv_taps.shape[1] // 2
    local_channels = w_value.shape[2]
    channels = local_channels * lax.axis_size("tp")
    tok_rows = tokens.shape[0]
    whole_value, whole_gate = (
        lax.all_gather(w_value, "sp", axis=1, tiled=True),
        lax.all_gather(w_gate, "sp", axis=1, tiled=True),
    )
    whole_out = lax.all_gather(w_out, "sp", axis=2, tiled=True)
    for layer_index in range(layer_count):
        whole_rows = lax.all_gather(stream, "tp", axis=1, tiled=True)
        rows_f32 = whole_rows.astype(jnp.float32)
        scale_rows = lax.rsqrt(jnp.mean(rows_f32 * rows_f32, axis=-1, keepdims=True) + norm_floor)
        normed = (rows_f32 * scale_rows * norm_gain[layer_index]).astype(jnp.bfloat16)
        value_rows = jnp.dot(normed, whole_value[layer_index], preferred_element_type=jnp.float32)
        gate_rows = jnp.dot(normed, whole_gate[layer_index], preferred_element_type=jnp.float32)
        gated_input = (value_rows * jax.nn.sigmoid(gate_rows)).astype(jnp.bfloat16)
        padded = with_halo(gated_input, (("sp", 0),), reach)
        padded = padded.astype(jnp.float32)
        convolved = jnp.zeros((tok_rows, local_channels), jnp.float32) + conv_bias[layer_index]
        for offset in range(2 * reach + 1):
            convolved = (
                convolved + conv_taps[layer_index, offset] * padded[offset : offset + tok_rows]
            )
        moments = lax.psum(
            (
                jnp.sum(convolved, axis=-1, keepdims=True),
                jnp.sum(convolved * convolved, axis=-1, keepdims=True),
            ),
            "tp",
        )
        average = moments[0] / channels
        spread = moments[1] / channels - average * average
        activated = jax.nn.silu(
            (convolved - average) * lax.rsqrt(spread + norm_floor) * ln_gain[layer_index]
            + ln_shift[layer_index]
        ).astype(jnp.bfloat16)
        partial_rows = jnp.dot(
            activated, whole_out[layer_index], preferred_element_type=jnp.float32
        )
        summed = lax.psum_scatter(
            partial_rows.astype(jnp.bfloat16), "tp", scatter_dimension=1, tiled=True
        ).astype(jnp.float32)
        stream = (stream.astype(jnp.float32) + summed).astype(jnp.bfloat16)
    return stream


def ring_order(layers, m):
    order = [(0, 0, 1), (0, 1, 1)]
    for layer in range(layers):
        order.append((layer, 2, 1))
        for step in range(2, m + 1):
            order += [(layer, 0, step), (layer, 1, step)]
        ahead = [(layer + 1, 0, 1), (layer + 1, 1, 1)] if layer + 1 < layers else []
        for step in range(2, m + 1):
            order.append((layer, 2, step))
            order += ahead[:1]
            ahead = ahead[1:]
        order += ahead
    if m > 2:
        last = layers - 1
        early = [(last, 2, step) for step in range(2, m - 1)]
        order = [e for e in order if e not in early]
        for e in early:
            order.insert(order.index((last, 1, e[2] + 1)), e)
    return order


def fused(
    dims,
    tok, gain_in, wv_in, wg_in, wo_in, taps_in, bias_in, lng_in, lns_in,
    out,
    wvg, wo, taps, bias, lng, lns, stream, gated, conv, acc1, acc2, act,
    part_out, part_in, stat_out, stat_in, stat_m, final_out, final_in,
    loc_sem, ring_send, ring_recv, pair_send, pair_recv,
    tok_send, tok_recv, halo_send, halo_recv, par_send, par_recv,
    px_send, px_recv, st_send, st_recv, fin_send, fin_recv,
):
    n, tp, layers, ntaps, rows, width, chans, pieces = dims
    feats = width // tp
    drows = width // n
    ocols = width // n
    lch = chans // tp
    pch = 2 * lch
    half_rows = rows // 2
    reach = ntaps // 2
    grain = 16
    halo = grain * layers
    window = half_rows + 2 * halo
    main = half_rows + halo
    m = n // 2
    half_feats = width // 2

    sp = lax.axis_index("sp")
    t = lax.axis_index("tp")
    h = lax.rem(t, 2)
    xg = t // 2
    pair = t + 1 - 2 * h
    across = lax.rem(t + 2, tp)
    odd = lax.rem(sp, 2)
    pos = (1 - odd) * (sp // 2) + odd * (n - (sp + 1) // 2)

    def ring_sp(p):
        p = lax.rem(p + 2 * n, n)
        q = p // m
        return (1 - q) * (2 * p) + q * (2 * (n - p) - 1)

    right, left = ring_sp(pos + 1), ring_sp(pos - 1)
    up, down = lax.rem(sp + 1, n), lax.rem(sp + n - 1, n)

    barrier = pltpu.get_barrier_semaphore()
    has_up, has_down = 1 - (sp + 1) // n, 1 - (n - sp) // n
    has_halo = (1 - h) * has_down + h * has_up
    greet = [(sp, lax.rem(t + j, tp)) for j in range(1, tp)]
    greet += [(right, t), (left, t)]

    def block(layer, kind, origin, side, half=None):
        part, count = (0, 1) if half is None else (half, 2)
        if kind < 2:
            size = drows // count
            r = pl.ds(pl.multiple_of(origin * drows + part * size, size), size)
            return wvg.at[layer, side, kind, r, :]
        size = lch // count
        c = pl.ds(pl.multiple_of(origin * ocols, ocols), ocols)
        return wo.at[layer, pl.ds(pl.multiple_of(side * lch + part * size, size), size), c]

    def local_copy(layer, kind):
        src = (wv_in, wg_in, wo_in)[kind].at[layer]
        return pltpu.make_async_copy(src, block(layer, kind, sp, h), loc_sem.at[3 * layer + kind])

    def ring_copy(layer, kind, direction, step):
        shift = -(step - 1) if direction == 0 else step - 1
        half = direction if step == m else None
        ref = block(layer, kind, ring_sp(pos + shift), h, half)
        i = ((layer * 3 + kind) * 2 + direction) * m + step - 1
        return pltpu.make_async_remote_copy(
            src_ref=ref, dst_ref=ref, send_sem=ring_send.at[i], recv_sem=ring_recv.at[i],
            device_id=(right if direction == 0 else left, t), device_id_type=MESH)

    def ring_arrival(layer, kind, direction, step, side):
        shift = -step if direction == 0 else step
        half = direction if step == m else None
        return block(layer, kind, ring_sp(pos + shift), side, half)

    def pair_copy(layer, kind, direction, step, side):
        if step == 0:
            ref, j = block(layer, kind, sp, side), 0
        else:
            ref, j = ring_arrival(layer, kind, direction, step, side), direction * m + step
        i = (layer * 3 + kind) * (2 * m + 1) + j
        return pltpu.make_async_remote_copy(
            src_ref=ref, dst_ref=ref, send_sem=pair_send.at[i], recv_sem=pair_recv.at[i],
            device_id=(sp, pair), device_id_type=MESH)

    sequence = ring_order(layers, m)
    place = {e: i for i, e in enumerate(sequence)}
    sent, handled = [0], [0]

    def pump():
        while sent[0] < len(sequence):
            layer, kind, step = sequence[sent[0]]
            if step > 1 and place[layer, kind, step - 1] >= handled[0]:
                return
            if step == 1:
                local_copy(layer, kind).wait()
            for d in range(2):
                ring_copy(layer, kind, d, step).start()
            if step == 1:
                pair_copy(layer, kind, 0, 0, h).start()
            sent[0] += 1

    def advance(upto):
        while handled[0] < min(upto, len(sequence)):
            layer, kind, step = sequence[handled[0]]
            for d in range(2):
                ref = ring_arrival(layer, kind, d, step, h)
                i = ((layer * 3 + kind) * 2 + d) * m + step - 1
                pltpu.make_async_remote_copy(
                    src_ref=ref, dst_ref=ref, send_sem=ring_send.at[i], recv_sem=ring_recv.at[i],
                    device_id=(right, t), device_id_type=MESH).wait_recv()
            handled[0] += 1
            pump()
            for d in range(2):
                pair_copy(layer, kind, d, step, h).start()

    def advance_by(count):
        advance(handled[0] + count)

    def need(layer, *kinds):
        advance(max(place[layer, k, m] for k in kinds) + 1)
        for k in kinds:
            pair_copy(layer, k, 0, 0, 1 - h).wait_recv()
            for step in range(1, m + 1):
                for d in range(2):
                    pair_copy(layer, k, d, step, 1 - h).wait_recv()

    tcols = pl.ds(pl.multiple_of(t * feats, feats), feats)

    def window_cols(owner):
        return pl.ds(pl.multiple_of(owner * feats, feats), feats)

    def tok_copy(j):
        dest = lax.rem(t + j, tp)
        dh = lax.rem(dest, 2)
        return pltpu.make_async_remote_copy(
            src_ref=tok.at[pl.ds(pl.multiple_of(dh * (rows - main), grain), main), :],
            dst_ref=stream.at[pl.ds(pl.multiple_of((1 - dh) * halo, grain), main), tcols],
            send_sem=tok_send.at[j - 1], recv_sem=tok_recv.at[j - 1],
            device_id=(sp, dest), device_id_type=MESH)

    def tok_wait(j):
        owner = lax.rem(t + tp - j, tp)
        ref = stream.at[pl.ds(pl.multiple_of((1 - h) * halo, grain), main), window_cols(owner)]
        return pltpu.make_async_remote_copy(
            src_ref=ref, dst_ref=ref, send_sem=tok_send.at[j - 1], recv_sem=tok_recv.at[j - 1],
            device_id=(sp, pair), device_id_type=MESH)

    def greet_halo(there, row):
        @pl.when(there == 1)
        def _():
            for c in range(2):
                pl.semaphore_signal(barrier, inc=1, device_id=(row, 2 * xg + c), device_id_type=MESH)

    def halo_copy(side):
        src, row, there = ((rows - halo, 0, up), (0, main, down))[side]
        return pltpu.make_async_remote_copy(
            src_ref=tok.at[pl.ds(src, halo), :], dst_ref=stream.at[pl.ds(row, halo), tcols],
            send_sem=halo_send.at[side], recv_sem=halo_recv.at[t],
            device_id=(there, 2 * xg + side), device_id_type=MESH)

    def halo_pass(group, c):
        owner = 2 * group + c
        ref = stream.at[pl.ds(pl.multiple_of(h * main, grain), halo), window_cols(owner)]
        return pltpu.make_async_remote_copy(
            src_ref=ref, dst_ref=ref, send_sem=halo_send.at[2 + c], recv_sem=halo_recv.at[owner],
            device_id=(sp, across), device_id_type=MESH)

    def halo_start():
        for side, there in enumerate((has_up, has_down)):
            pl.when(there == 1)(lambda side=side: halo_copy(side).start())

    def halo_forward():
        @pl.when(has_halo == 1)
        def _():
            for c in range(2):
                halo_pass(xg, c).wait_recv()
                halo_pass(xg, c).start()

        @pl.when(has_halo == 0)
        def _():
            stream[pl.ds(pl.multiple_of(h * main, grain), halo), :] = jnp.zeros((halo, width), jnp.bfloat16)

    def halo_finish():
        @pl.when(has_halo == 1)
        def _():
            for c in range(2):
                halo_pass(1 - xg, c).wait_recv()
                halo_pass(xg, c).wait_send()

    def halo_sent():
        for side, there in enumerate((has_up, has_down)):
            pl.when(there == 1)(lambda side=side: halo_copy(side).wait_send())

    def param_copies():
        for i, (a, b) in enumerate(((taps_in, taps), (bias_in, bias), (lng_in, lng), (lns_in, lns))):
            yield pltpu.make_async_remote_copy(
                src_ref=a, dst_ref=b.at[h], send_sem=par_send.at[i], recv_sem=par_recv.at[i],
                device_id=(sp, pair), device_id_type=MESH)

    def param_waits():
        for i, (a, b) in enumerate(((taps_in, taps), (bias_in, bias), (lng_in, lng), (lns_in, lns))):
            yield pltpu.make_async_remote_copy(
                src_ref=a, dst_ref=b.at[1 - h], send_sem=par_send.at[i], recv_sem=par_recv.at[i],
                device_id=(sp, pair), device_id_type=MESH)

    for layer in range(layers):
        for kind in range(3):
            local_copy(layer, kind).start()
    for dev in greet:
        pl.semaphore_signal(barrier, inc=1, device_id=dev, device_id_type=MESH)
    greet_halo(has_up, up)
    greet_halo(has_down, down)
    pl.semaphore_wait(barrier, len(greet) + 2 * (has_up + has_down))

    pump()
    for j in range(1, tp):
        tok_copy(j).start()
    halo_start()
    for c in param_copies():
        c.start()

    stream[pl.ds(pl.multiple_of((1 - h) * halo, grain), main), tcols] = tok[
        pl.ds(pl.multiple_of(h * (rows - main), grain), main), :]
    taps[h] = taps_in[...]
    bias[h] = bias_in[...]
    lng[h] = lng_in[...]
    lns[h] = lns_in[...]
    stat_m[...] = jnp.zeros_like(stat_m)

    first_row = sp * rows + h * half_rows - halo
    total_rows = n * rows

    def project(layer, start, size):
        x = stream[pl.ds(start, size), :].astype(jnp.float32)
        scale = lax.rsqrt(jnp.mean(x * x, axis=-1, keepdims=True) + norm_floor)
        normed = (x * scale * gain_in[layer:layer + 1, :]).astype(jnp.bfloat16)
        row = lax.broadcasted_iota(jnp.int32, (size, lch), 0) + (first_row + start)
        inside = jnp.logical_and(row >= 0, row < total_rows)
        for c in range(2):
            value = jnp.dot(normed, wvg[layer, c, 0], preferred_element_type=jnp.float32)
            gate = jnp.dot(normed, wvg[layer, c, 1], preferred_element_type=jnp.float32)
            g = (value * jax.nn.sigmoid(gate)).astype(jnp.bfloat16).astype(jnp.float32)
            gated[pl.ds(start, size), c * lch:(c + 1) * lch] = jnp.where(inside, g, 0.0)

    def convolve(layer, start, r0, size):
        lanes_per = 128
        per_side = lch // lanes_per
        acc1[...] = jnp.zeros_like(acc1)
        acc2[...] = jnp.zeros_like(acc2)

        def lane_block(b, carry):
            c = b // per_side
            lane = pl.ds(pl.multiple_of(lax.rem(b, per_side) * lanes_per, lanes_per), lanes_per)
            wide = pl.ds(pl.multiple_of(b * lanes_per, lanes_per), lanes_per)
            total = jnp.zeros((size, lanes_per), jnp.float32) + bias[c, layer:layer + 1, lane]
            for k in range(ntaps):
                first = start + r0 + k - reach
                total = total + taps[c, layer, k:k + 1, lane] * gated[first:first + size, wide]
            conv[r0:r0 + size, wide] = total
            acc1[0:size, :] += total
            acc2[0:size, :] += total * total
            return carry

        lax.fori_loop(0, 2 * per_side, lane_block, 0)

    def send_stats(layer, i, size):
        lane_id = lax.broadcasted_iota(jnp.int32, (size, 128), 1)
        s1 = jnp.sum(acc1[0:size, :], axis=-1, keepdims=True)
        s2 = jnp.sum(acc2[0:size, :], axis=-1, keepdims=True)
        stat_m[0:size, :] = jnp.where(lane_id == 0, s1, jnp.where(lane_id == 1, s2, 0.0))
        stat_out[layer * pieces + i] = jnp.transpose(stat_m[...])[0:8, :]
        stat_copy(layer * pieces + i).start()

    def stat_copy(layer):
        return pltpu.make_async_remote_copy(
            src_ref=stat_out.at[layer], dst_ref=stat_in.at[layer], send_sem=st_send.at[layer],
            recv_sem=st_recv.at[layer], device_id=(sp, across), device_id_type=MESH)

    def part_copy(layer, i, r0, size, last):
        r = pl.ds(r0, size)
        if last:
            src = part_out.at[layer, r, pl.ds(pl.multiple_of((1 - xg) * half_feats, half_feats), half_feats)]
            dst = part_in.at[layer, r, pl.ds(pl.multiple_of((1 - xg) * half_feats, half_feats), half_feats)]
        else:
            src, dst = part_out.at[layer, r, :], part_in.at[layer, r, :]
        return pltpu.make_async_remote_copy(
            src_ref=src, dst_ref=dst, send_sem=px_send.at[layer * pieces + i],
            recv_sem=px_recv.at[layer * pieces + i], device_id=(sp, across), device_id_type=MESH)

    def finish_sends():
        halo_sent()
        for j in range(1, tp):
            tok_copy(j).wait_send()
        for c in param_copies():
            c.wait_send()
        for layer in range(layers):
            piece = (window - 2 * grain * (layer + 1)) // pieces
            for i in range(pieces):
                stat_copy(layer * pieces + i).wait_send()
                if layer < layers - 1:
                    part_copy(layer, i, i * piece, piece, False).wait_send()
            for kind in range(3):
                pair_copy(layer, kind, 0, 0, h).wait_send()
                for step in range(1, m + 1):
                    for d in range(2):
                        ring_copy(layer, kind, d, step).wait_send()
                        pair_copy(layer, kind, d, step, h).wait_send()

    advance(3)
    halo_forward()
    advance(max(place[0, 0, m], place[0, 1, m]) + 1)
    for j in range(1, tp):
        tok_wait(j).wait_recv()
    halo_finish()
    need(0, 0, 1)
    for i in range(2):
        project(0, i * (window // 2), window // 2)
    advance_by(1)
    for c in param_waits():
        c.wait_recv()

    for layer in range(layers):
        last = layer == layers - 1
        start = grain * (layer + 1)
        size = window - 2 * start
        piece = size // pieces
        for i in range(pieces):
            convolve(layer, start, i * piece, piece)
            send_stats(layer, i, piece)
            advance_by(1)
        need(layer, 2)
        for i in range(pieces):
            r0 = i * piece
            j = layer * pieces + i
            stat_copy(j).wait_recv()
            both = stat_out[j] + stat_in[j]
            wide = jnp.concatenate([both, jnp.zeros((120, both.shape[1]), jnp.float32)], axis=0)
            sums = jnp.transpose(wide)
            average = sums[0:piece, 0:1] / chans
            spread = sums[0:piece, 1:2] / chans - average * average
            scale = lax.rsqrt(spread + norm_floor)
            for c in range(2):
                y = (conv[r0:r0 + piece, c * lch:(c + 1) * lch] - average) * scale
                y = y * lng[c, layer:layer + 1, :] + lns[c, layer:layer + 1, :]
                act[r0:r0 + piece, c * lch:(c + 1) * lch] = (y / (1.0 + jnp.exp(-y))).astype(jnp.bfloat16)
            part_out[layer, r0:r0 + piece, :] = jnp.dot(
                act[r0:r0 + piece, :], wo[layer], preferred_element_type=jnp.float32).astype(jnp.bfloat16)
            part_copy(layer, i, r0, piece, last).start()
        if not last:
            need(layer + 1, 0, 1)
            for i in range(pieces):
                r0 = i * piece
                part_copy(layer, i, r0, piece, last).wait_recv()
                w0 = start + r0
                stream[w0:w0 + piece, :] = (
                    stream[w0:w0 + piece, :].astype(jnp.float32)
                    + part_out[layer, r0:r0 + piece, :].astype(jnp.float32)
                    + part_in[layer, r0:r0 + piece, :].astype(jnp.float32)).astype(jnp.bfloat16)
                project(layer + 1, w0, piece)
                advance_by(1)
        else:
            finish_sends()
            mycols = pl.ds(pl.multiple_of(xg * half_feats, half_feats), half_feats)

            def fin_copy(i, r0):
                return pltpu.make_async_remote_copy(
                    src_ref=final_out.at[pl.ds(r0, piece), pl.ds(pl.multiple_of((1 - h) * feats, feats), feats)],
                    dst_ref=final_in.at[pl.ds(r0, piece), :],
                    send_sem=fin_send.at[i], recv_sem=fin_recv.at[i],
                    device_id=(sp, pair), device_id_type=MESH)

            for i in range(pieces):
                r0 = i * piece
                ref = part_in.at[layer, pl.ds(r0, piece), mycols]
                pltpu.make_async_remote_copy(
                    src_ref=ref, dst_ref=ref, send_sem=px_send.at[layer * pieces + i],
                    recv_sem=px_recv.at[layer * pieces + i], device_id=(sp, across),
                    device_id_type=MESH).wait_recv()
                w0 = start + r0
                final_out[r0:r0 + piece, :] = (
                    stream[w0:w0 + piece, mycols].astype(jnp.float32)
                    + part_out[layer, r0:r0 + piece, mycols].astype(jnp.float32)
                    + part_in[layer, r0:r0 + piece, mycols].astype(jnp.float32)).astype(jnp.bfloat16)
                fin_copy(i, r0).start()
            out[pl.ds(pl.multiple_of(h * half_rows, grain), half_rows), :] = final_out[
                :, pl.ds(pl.multiple_of(h * feats, feats), feats)]
            for i in range(pieces):
                fin_copy(i, i * piece).wait_recv()
            out[pl.ds(pl.multiple_of((1 - h) * half_rows, grain), half_rows), :] = final_in[...]
            for i in range(pieces):
                fin_copy(i, i * piece).wait_send()
    for i in range(pieces):
        part_copy(layers - 1, i, i * (half_rows // pieces), half_rows // pieces, True).wait_send()


def fused_call(mesh, *args):
    tokens, norm_gain, w_value, w_gate, conv_taps, conv_bias, ln_gain, ln_shift, w_out = args
    n, tp = mesh.shape["sp"], mesh.shape["tp"]
    layers, ntaps, lch = conv_taps.shape
    rows, feats = tokens.shape
    width, chans = feats * tp, lch * tp
    pieces = 2
    half_rows = rows // 2
    window = half_rows + 32 * layers
    most = window - 32
    stat_rows = -(-most // pieces // 128) * 128
    m = n // 2
    dims = (n, tp, layers, ntaps, rows, width, chans, pieces)
    vmem = pl.BlockSpec(memory_space=pltpu.VMEM)
    anys = pl.BlockSpec(memory_space=pl.ANY)
    bf, f32 = jnp.bfloat16, jnp.float32
    dma = lambda k: pltpu.SemaphoreType.DMA((k,))
    ring_sems = layers * 3 * 2 * m
    pair_sems = layers * 3 * (2 * m + 1)
    return pl.pallas_call(
        functools.partial(fused, dims),
        out_shape=jax.ShapeDtypeStruct((rows, feats), bf),
        in_specs=[vmem, vmem, anys, anys, anys, vmem, vmem, vmem, vmem],
        out_specs=vmem,
        scratch_shapes=[
            pltpu.VMEM((layers, 2, 2, width, lch), bf),
            pltpu.VMEM((layers, 2 * lch, width), bf),
            pltpu.VMEM((2,) + conv_taps.shape, f32),
            pltpu.VMEM((2,) + conv_bias.shape, f32),
            pltpu.VMEM((2,) + ln_gain.shape, f32),
            pltpu.VMEM((2,) + ln_shift.shape, f32),
            pltpu.VMEM((window, width), bf),
            pltpu.VMEM((window, 2 * lch), f32),
            pltpu.VMEM((most, 2 * lch), f32),
            pltpu.VMEM((most // pieces, 128), f32),
            pltpu.VMEM((most // pieces, 128), f32),
            pltpu.VMEM((most, 2 * lch), bf),
            pltpu.VMEM((layers, most, width), bf),
            pltpu.VMEM((layers, most, width), bf),
            pltpu.VMEM((layers * pieces, 8, stat_rows), f32),
            pltpu.VMEM((layers * pieces, 8, stat_rows), f32),
            pltpu.VMEM((stat_rows, 128), f32),
            pltpu.VMEM((half_rows, 2 * feats), bf),
            pltpu.VMEM((half_rows, feats), bf),
            dma(3 * layers), dma(ring_sems), dma(ring_sems), dma(pair_sems), dma(pair_sems),
            dma(tp - 1), dma(tp - 1), dma(tp), dma(tp), dma(4), dma(4),
            dma(layers * pieces), dma(layers * pieces), dma(layers * pieces), dma(layers * pieces),
            dma(pieces), dma(pieces),
        ],
        compiler_params=pltpu.CompilerParams(
            collective_id=0, has_side_effects=True, vmem_limit_bytes=60 * 1024 * 1024),
    )(tokens, norm_gain, w_value, w_gate, w_out, conv_taps, conv_bias, ln_gain, ln_shift)


def fits(mesh, tokens, conv_taps, w_out):
    n, tp = mesh.shape["sp"], mesh.shape["tp"]
    layers, ntaps, lch = conv_taps.shape
    rows, feats = tokens.shape
    sizes = [rows // 2 + 32 * (layers - 1 - i) for i in range(layers)]
    return (tp == 4 and n % 2 == 0 and n >= 4 and ntaps % 2 == 1 and ntaps // 2 < 16
            and w_out.shape[2] % 128 == 0 and lch % 256 == 0 and feats % 128 == 0
            and rows % 32 == 0 and rows // 2 >= 16 * layers
            and all(s % 32 == 0 and s <= 256 for s in sizes)
            and layers * w_out.shape[1] * w_out.shape[2] * n * 12 <= 20 * 1024 * 1024)


def solution(mesh):
    placed = (
        P("sp", "tp"),
        P(),
        P(None, "sp", "tp"),
        P(None, "sp", "tp"),
        P(None, None, "tp"),
        P(None, "tp"),
        P(None, "tp"),
        P(None, "tp"),
        P(None, "tp", "sp"),
    )

    def run(*args):
        if fits(mesh, args[0], args[4], args[8]):
            return fused_call(mesh, *args)
        return body(*args)

    return jax.shard_map(run, mesh=mesh, in_specs=placed, out_specs=P("sp", "tp"), check_vma=False)
```
